32 devices in a mesh: rep: 2 (over y), fs: 4 (over z), tp: 4 (over x, core).
Axes of the slice: x: 2, y: 2, z: 4, core: 2. Of those that a mesh axis runs over, the one named last changes fastest.
Arguments:
- activations: bfloat16 [2048, 4096], P(None, ('rep', 'fs')), may hold values from -60 to 60
- w_mix_in: bfloat16 [2048, 1024], P('fs', 'tp'), may hold values from -0.125 to 0.125
- w_mix_out: bfloat16 [2048, 1024], P('fs', 'tp'), may hold values from -0.1875 to 0.1875
- w_gate: bfloat16 [2048, 2816], P('fs', 'tp'), may hold values from -0.125 to 0.125
- w_up: bfloat16 [2048, 2816], P('fs', 'tp'), may hold values from -0.125 to 0.125
- w_down: bfloat16 [2048, 2816], P('fs', 'tp'), may hold values from -0.109375 to 0.109375
- pool_scale: float32 [1024], replicated, may hold values from 0.1 to 1.9
- gain_mix: float32 [2048], replicated, may hold values from 0.1 to 1.9
- gain_ffn: float32 [2048], replicated, may hold values from 0.1 to 1.9
- gain_out: float32 [2048], replicated, may hold values from 0.1 to 1.9
Outputs:
- normalized: bfloat16 [2048, 4096], P('tp', ('rep', 'fs'))
The draws below stay inside these ranges and needn't reach their ends.
All inputs are finite; a program needn't handle non-finite values.
Results may differ from the reference program's by a relative error of at most 0.014.
Values may be sent and summed in bfloat16 or wider, within the bound.
A program may use at most 64 MiB of HBM per device.

```python
import jax
import jax.numpy as jnp
from jax import lax

D = 2048
BRANCH = 1024
FF = 2816
POOL_GROUP = 256
SEQ_LEN = 256
TOKENS = 4096
N_TP = 4


def draw_activations(key, part):
    key_rough, key_noise = jax.random.split(key, 2)
    feature_place = jnp.arange(D, dtype=jnp.float32)[:, None] / D
    rough = jax.random.uniform(key_rough, (D, 1), jnp.float32, -0.3, 0.3)
    feature_scale = 0.5 * jnp.exp(jnp.log(8.0) * feature_place + rough)
    values = jnp.clip(jax.random.normal(key_noise, (D, TOKENS), jnp.float32), -6.0, 6.0)
    return jnp.clip(values * feature_scale, -60.0, 60.0).astype(jnp.bfloat16)


def levels(own_key, shape, shards, smallest, top_value):
    def one(axis_at, blocks):
        draws = jax.random.uniform(jax.random.fold_in(jax.random.fold_in(own_key, 6), axis_at), (blocks,), jnp.float32, smallest / len(shards), top_value / len(shards))
        return jnp.repeat(jnp.exp(draws), shape[axis_at] // blocks).reshape((-1,) + (1,) * (len(shape) - axis_at - 1))

    gain = one(*shards[0])
    for cut in shards[1:]:
        gain = gain * one(*cut)
    return gain


def gaussian(rng, shape, scale, reach, shards=(), kind=jnp.bfloat16):
    drawn = scale * jax.random.normal(rng, shape, jnp.float32)
    if shards:
        drawn = drawn * levels(rng, shape, shards, -0.22, 0.18)
    return jnp.clip(drawn, -reach, reach).astype(kind)


def setup_inputs(seed: int = 0) -> dict:
    key_list = jax.random.split(jax.random.key(seed), 11)
    activations = draw_activations(jax.random.fold_in(key_list[10], 71), 0)
    w_mix_in = gaussian(key_list[1], (D, BRANCH), D ** -0.5, 0.125, ((0, 4), (1, 4)))
    w_mix_out = gaussian(key_list[2], (D, BRANCH), BRANCH ** -0.5, 0.1875, ((0, 4), (1, 4)))
    w_gate = gaussian(key_list[3], (D, FF), D ** -0.5, 0.125, ((0, 4), (1, 4)))
    w_up = gaussian(key_list[4], (D, FF), D ** -0.5, 0.125, ((0, 4), (1, 4)))
    w_down = gaussian(key_list[5], (D, FF), FF ** -0.5, 0.109375, ((0, 4), (1, 4)))
    pool_scale = jnp.clip(1.0 + 0.18 * jax.random.normal(key_list[6], (BRANCH,), jnp.float32), 0.1, 1.9)
    gain_mix = jnp.clip(1.0 + 0.18 * jax.random.normal(key_list[7], (D,), jnp.float32), 0.1, 1.9)
    gain_ffn = jnp.clip(1.0 + 0.18 * jax.random.normal(key_list[8], (D,), jnp.float32), 0.1, 1.9)
    gain_out = jnp.clip(1.0 + 0.18 * jax.random.normal(key_list[9], (D,), jnp.float32), 0.1, 1.9)
    return {"activations": activations, "w_mix_in": w_mix_in, "w_mix_out": w_mix_out, "w_gate": w_gate, "w_up": w_up, "w_down": w_down, "pool_scale": pool_scale, "gain_mix": gain_mix, "gain_ffn": gain_ffn, "gain_out": gain_out}


EPS = 1e-06
WINDOWS = (2, 4, 8, 16)

def rms_factor(stream):
    return lax.rsqrt(lax.optimization_barrier(jnp.mean(stream * stream, axis=0, keepdims=True)) + EPS)

def pool_tokens(inputs, group_of):
    channels = inputs.shape[0]
    values = inputs.astype(jnp.float32).reshape(channels, -1, SEQ_LEN)
    sequences = values.shape[1]
    running = jnp.concatenate([jnp.zeros((channels, sequences, 1), jnp.float32), jnp.cumsum(values, axis=-1)], axis=-1)
    places = jnp.arange(SEQ_LEN, dtype=jnp.int32)
    pooled_sum = jnp.zeros_like(values)
    for group_id, window in enumerate(WINDOWS):
        behind = window // 2
        onward = window - behind
        upper_sum = jnp.concatenate([running, jnp.repeat(running[..., -1:], onward, axis=-1)], axis=-1)[..., onward:onward + SEQ_LEN]
        lower_sum = jnp.concatenate([jnp.zeros((channels, sequences, behind), jnp.float32), running], axis=-1)[..., :SEQ_LEN]
        counts = (jnp.minimum(places + onward, SEQ_LEN) - jnp.maximum(places - behind, 0)).astype(jnp.float32)
        window_mean = (upper_sum - lower_sum) / counts
        pooled_sum = pooled_sum + jnp.where((group_of == group_id)[:, None, None], window_mean, 0.0)
    return (pooled_sum - values).reshape(channels, -1)

def block_sum(weights, acts, blocks):
    width = acts.shape[0] // blocks
    stacked_weights = jnp.transpose(weights.reshape(weights.shape[0], blocks, width), (1, 0, 2))
    stacked_acts = acts.reshape(blocks, width, acts.shape[1])

    def add_block(carry, pair):
        term = jnp.dot(pair[0], pair[1], preferred_element_type=jnp.float32).astype(jnp.bfloat16)
        term = lax.optimization_barrier(term)
        return (carry + term.astype(jnp.float32), None)
    start = jnp.zeros((weights.shape[0], acts.shape[1]), jnp.float32)
    total, _ = lax.scan(add_block, start, (stacked_weights, stacked_acts))
    return total

def reference(activations, w_mix_in, w_mix_out, w_gate, w_up, w_down, pool_scale, gain_mix, gain_ffn, gain_out):
    stream = activations.astype(jnp.float32)
    normed = (stream * rms_factor(stream) * gain_mix[:, None]).astype(jnp.bfloat16)
    inputs = jnp.dot(w_mix_in.T, normed, preferred_element_type=jnp.float32).astype(jnp.bfloat16)
    group_of = (jnp.arange(BRANCH, dtype=jnp.int32) // POOL_GROUP).astype(jnp.int32)
    pooled = (pool_tokens(inputs, group_of) * pool_scale[:, None]).astype(jnp.bfloat16)
    mixed = block_sum(w_mix_out, pooled, N_TP)
    after_mix = lax.optimization_barrier((stream + mixed).astype(jnp.bfloat16)).astype(jnp.float32)
    normed_two = (after_mix * rms_factor(after_mix) * gain_ffn[:, None]).astype(jnp.bfloat16)
    gate = jnp.dot(w_gate.T, normed_two, preferred_element_type=jnp.float32)
    upward = jnp.dot(w_up.T, normed_two, preferred_element_type=jnp.float32)
    hidden = (jax.nn.silu(gate) * upward).astype(jnp.bfloat16)
    ffn_out = block_sum(w_down, hidden, N_TP)
    final = after_mix + ffn_out
    return (final * rms_factor(final) * gain_out[:, None]).astype(jnp.bfloat16)
```

```python
import functools

import jax
import jax.numpy as jnp
from jax import lax
from jax.experimental import pallas as pl
from jax.experimental.pallas import tpu as pltpu
from jax.sharding import PartitionSpec as P

POOL_GROUP = 256
SEQ_LEN = 256
EPS = 1e-06
LANES = 128
MESH = pl.DeviceIdType.MESH
BF = jnp.bfloat16
F32 = jnp.float32


def dot_first(weights, acts):
    return lax.dot_general(weights, acts, (((0,), (0,)), ((), ())), preferred_element_type=F32)


def column(row, width):
    square = jnp.transpose(jnp.broadcast_to(row, (LANES, LANES)))
    return jnp.concatenate([square] * (width // LANES), axis=1)


def body(
    nr, nf, nt,
    act, w_in, w_out, w_gate, w_up, w_down, scale, g_mix, g_ffn, g_out, out,
    b_in, b_out, b_gate, b_up, b_down,
    h, x1, part0, part1, u_acc, pooled, gate_acc, up_acc, hidden, own_x, squares,
    buf_a, buf_b,
    own_sem, zsend, zrecv, ysend, yrecv,
    a_send, a_recv, b_send, b_recv, c_send, c_recv, d_send, d_recv, s_send, s_recv,
):
    r, f, t = lax.axis_index("rep"), lax.axis_index("fs"), lax.axis_index("tp")
    features, tokens = act.shape
    shards = (w_in, w_out, w_gate, w_up, w_down)
    full = (b_in, b_out, b_gate, b_up, b_down)
    rows = w_in.shape[0]
    piece = rows // nr
    share = features // nt
    channels = w_in.shape[1]
    ff = w_gate.shape[1]
    nh = nt // 2
    chip, parity = t // 2, lax.rem(t, 2)
    partner = t + 1 - 2 * parity

    own = [pltpu.make_async_copy(shards[m], full[m].at[f], own_sem.at[m]) for m in range(5)]
    for copy in own:
        copy.start()

    barrier = pltpu.get_barrier_semaphore()
    for step in (1, nf - 1):
        pl.semaphore_signal(barrier, inc=1, device_id=(r, lax.rem(f + step, nf), t), device_id_type=MESH)
    for o in range(1, nr):
        pl.semaphore_signal(barrier, inc=1, device_id=(lax.rem(r + o, nr), f, t), device_id_type=MESH)
    for i in range(1, nt):
        pl.semaphore_signal(barrier, inc=1, device_id=(r, f, lax.rem(t + i, nt)), device_id_type=MESH)
    pl.semaphore_wait(barrier, 2 + (nr - 1) + (nt - 1))

    def z_copy(m, blk, way, d):
        ref = full[m].at[blk, pl.ds(pl.multiple_of(r * piece, piece), piece), :]
        return pltpu.make_async_remote_copy(
            src_ref=ref, dst_ref=ref,
            send_sem=zsend.at[m, way, lax.rem(d, 2)], recv_sem=zrecv.at[m, blk],
            device_id=(r, f + 1 - 2 * way, t), device_id_type=MESH,
        )

    def y_copy(m, blk, way, d, o):
        ref = full[m].at[blk, pl.ds(pl.multiple_of(r * piece, piece), piece), :]
        return pltpu.make_async_remote_copy(
            src_ref=ref, dst_ref=ref,
            send_sem=ysend.at[m, way, lax.rem(d, 2), o - 1], recv_sem=yrecv.at[m, blk, o - 1],
            device_id=(lax.rem(r + o, nr), f, t), device_id_type=MESH,
        )

    def y_arrival(m, blk, o):
        source = lax.rem(r - o + nr, nr)
        ref = full[m].at[blk, pl.ds(pl.multiple_of(source * piece, piece), piece), :]
        return pltpu.make_async_remote_copy(
            src_ref=ref, dst_ref=ref,
            send_sem=ysend.at[m, 0, 0, o - 1], recv_sem=yrecv.at[m, blk, o - 1],
            device_id=(lax.rem(r + o, nr), f, t), device_id_type=MESH,
        )

    can_send = (f + 1 < nf, f >= 1)
    hops = (f, nf - 1 - f)

    def send_own(m):
        own[m].wait()
        for way in (0, 1):
            @pl.when(can_send[way])
            def _():
                z_copy(m, f, way, 0).start()

    def arrival(m, way, d):
        blk = f - d if way == 0 else f + d

        @pl.when(d <= hops[way])
        def _():
            z_copy(m, blk, way, d).wait_recv()

            @pl.when(can_send[way])
            def _():
                @pl.when(d >= 2)
                def _():
                    z_copy(m, blk, way, d).wait_send()

                z_copy(m, blk, way, d).start()

            for o in range(1, nr):
                @pl.when(d >= 3)
                def _():
                    y_copy(m, blk, way, d, o).wait_send()

                y_copy(m, blk, way, d, o).start()

    def gather(m, low, high):
        if low >= high:
            return

        def rounds(d, carry):
            arrival(m, 0, d)
            arrival(m, 1, d)
            return carry

        if low == 1:
            rounds(jnp.int32(1), 0)
            if m + 2 < 5:
                send_own(m + 2)
            low = 2
        lax.fori_loop(low, high, rounds, 0)

    def finish(m):
        def one(blk, carry):
            @pl.when(blk != f)
            def _():
                for o in range(1, nr):
                    y_arrival(m, blk, o).wait_recv()
            return carry

        lax.fori_loop(0, nf, one, 0)

    def drain(m):
        for way in (0, 1):
            for back in (0, 1):
                last = hops[way] - back

                @pl.when(jnp.logical_and(can_send[way], last >= 0))
                def _():
                    z_copy(m, f, way, last).wait_send()

                @pl.when(last >= 1)
                def _():
                    for o in range(1, nr):
                        y_copy(m, f, way, last, o).wait_send()

    def share_of(ref, j):
        return ref.at[pl.ds(pl.multiple_of(j * share, share), share), :]

    def normalize(load, gain, store, count):
        def square(i, total):
            v = load(i)
            return total + jnp.sum(v * v, axis=0, keepdims=True)

        total = lax.fori_loop(0, count, square, jnp.zeros((1, tokens), F32))
        factor = lax.rsqrt(total / features + EPS)

        def scaled(i, carry):
            store(i, load(i) * factor * column(gain[pl.ds(i, 1), :], tokens))
            return carry

        lax.fori_loop(0, count, scaled, 0)

    def chunk(ref, i):
        return ref[pl.ds(pl.multiple_of(i * LANES, LANES), LANES), :].astype(F32)

    def put(ref):
        def store(i, v):
            ref[pl.ds(pl.multiple_of(i * LANES, LANES), LANES), :] = v.astype(ref.dtype)
        return store

    def a_copy(k, part, c):
        return pltpu.make_async_remote_copy(
            src_ref=share_of(part, 2 * c + 1 - parity), dst_ref=buf_a.at[k, c],
            send_sem=a_send.at[k, c], recv_sem=a_recv.at[k, c],
            device_id=(r, f, partner), device_id_type=MESH,
        )

    def b_copy(k, part, i):
        target = 2 * lax.rem(chip + i, nh) + parity
        return pltpu.make_async_remote_copy(
            src_ref=share_of(part, target), dst_ref=buf_b.at[k, i],
            send_sem=b_send.at[k, i], recv_sem=b_recv.at[k, i],
            device_id=(r, f, target), device_id_type=MESH,
        )

    def start_pair(k, part):
        for i in range(nh):
            a_copy(k, part, i).start()

    def start_chips(k, part):
        for c in range(nh):
            a_copy(k, part, c).wait()
        for i in range(1, nh):
            c = lax.rem(chip + i, nh)
            target = 2 * c + parity

            def add(n, carry):
                at = pl.ds(pl.multiple_of(target * share + n * LANES, LANES), LANES)
                mine = part[at, :].astype(F32)
                theirs = buf_a[k, c, pl.ds(pl.multiple_of(n * LANES, LANES), LANES), :].astype(F32)
                part[at, :] = (mine + theirs).astype(BF)
                return carry

            lax.fori_loop(0, share // LANES, add, 0)
            b_copy(k, part, i).start()

    def finish_chips(k, part, base, store):
        for i in range(1, nh):
            b_copy(k, part, i).wait()

        def add(n, carry):
            here = pl.ds(pl.multiple_of(n * LANES, LANES), LANES)
            at = pl.ds(pl.multiple_of(t * share + n * LANES, LANES), LANES)
            total = part[at, :].astype(F32) + buf_a[k, chip, here, :].astype(F32)
            for i in range(1, nh):
                total = total + buf_b[k, i, here, :].astype(F32)
            store(n, base[at, :].astype(F32) + total)
            return carry

        lax.fori_loop(0, share // LANES, add, 0)

    def c_copy(i):
        ref = share_of(x1, t)
        return pltpu.make_async_remote_copy(
            src_ref=ref, dst_ref=ref, send_sem=c_send.at[i], recv_sem=c_recv.at[i],
            device_id=(r, f, 2 * lax.rem(chip + i, nh) + parity), device_id_type=MESH,
        )

    def d_copy(i):
        ref = share_of(x1, 2 * lax.rem(chip - i + nh, nh) + parity)
        return pltpu.make_async_remote_copy(
            src_ref=ref, dst_ref=ref, send_sem=d_send.at[i], recv_sem=d_recv.at[i],
            device_id=(r, f, partner), device_id_type=MESH,
        )

    def s_copy(i):
        return pltpu.make_async_remote_copy(
            src_ref=squares.at[0], dst_ref=squares.at[i], send_sem=s_send.at[i], recv_sem=s_recv.at[i],
            device_id=(r, f, lax.rem(t + i, nt)), device_id_type=MESH,
        )

    send_own(0)
    send_own(1)
    normalize(functools.partial(chunk, act), g_mix, put(h), features // LANES)

    gather(0, 1, nf)
    finish(0)
    u_acc[...] = jnp.zeros_like(u_acc)

    def mix_in(b, carry):
        at = pl.ds(pl.multiple_of(b * rows, rows), rows)
        u_acc[...] += dot_first(b_in[b], h[at, :])
        return carry

    lax.fori_loop(0, nf, mix_in, 0)
    for i in range(channels // LANES):
        first = t * channels + i * LANES
        window = jnp.int32(2) << (first // POOL_GROUP)
        behind = window // 2
        onward = window - behind
        source = lax.broadcasted_iota(jnp.int32, (SEQ_LEN, SEQ_LEN), 0)
        place = lax.broadcasted_iota(jnp.int32, (SEQ_LEN, SEQ_LEN), 1)
        inside = jnp.logical_and(source >= place - behind, source < place + onward)
        band = jnp.where(inside, 1.0, 0.0).astype(BF)
        spot = lax.broadcasted_iota(jnp.int32, (1, SEQ_LEN), 1)
        count = (jnp.minimum(spot + onward, SEQ_LEN) - jnp.maximum(spot - behind, 0)).astype(F32)
        gain = column(scale[pl.ds(first // LANES, 1), :], SEQ_LEN)
        for s in range(tokens // SEQ_LEN):
            at = (pl.ds(i * LANES, LANES), pl.ds(s * SEQ_LEN, SEQ_LEN))
            u = u_acc[at].astype(BF)
            mean = jnp.dot(u, band, preferred_element_type=F32) / count
            pooled[at] = ((mean - u.astype(F32)) * gain).astype(BF)

    gather(1, 1, nf)
    finish(1)

    def mix_out(b, carry):
        at = pl.ds(pl.multiple_of(b * rows, rows), rows)
        part0[at, :] = jnp.dot(b_out[b], pooled[...], preferred_element_type=F32).astype(BF)
        return carry

    lax.fori_loop(0, nf, mix_out, 0)
    start_pair(0, part0)
    third = 1 + (nf - 1) // 3
    gather(2, 1, third)
    start_chips(0, part0)
    gather(2, third, nf)

    def keep_x1(n, v):
        at = pl.ds(pl.multiple_of(t * share + n * LANES, LANES), LANES)
        x1[at, :] = v.astype(BF)

    finish_chips(0, part0, act, keep_x1)
    for i in range(1, nh):
        c_copy(i).start()
    d_copy(0).start()
    far = 1 + 2 * (nf - 1) // 3
    gather(3, 1, far)
    for i in range(1, nh):
        c_copy(i).wait()
        d_copy(i).start()
    gather(3, far, nf)
    for i in range(nh):
        d_copy(i).wait()
    normalize(functools.partial(chunk, x1), g_ffn, put(h), features // LANES)
    finish(2)
    gate_acc[...] = jnp.zeros_like(gate_acc)
    up_acc[...] = jnp.zeros_like(up_acc)

    def project(source, acc):
        def one(b, carry):
            at = pl.ds(pl.multiple_of(b * rows, rows), rows)
            acc[...] += dot_first(source[b], h[at, :])
            return carry

        lax.fori_loop(0, nf, one, 0)

    project(b_gate, gate_acc)
    gather(4, 1, third)
    finish(3)
    project(b_up, up_acc)
    gather(4, third, far)
    step = 32

    def activate(n, carry):
        at = pl.ds(pl.multiple_of(n * step, step), step)
        v = gate_acc[at, :]
        hidden[at, :] = (v / (1.0 + jnp.exp(-v)) * up_acc[at, :]).astype(BF)
        return carry

    lax.fori_loop(0, ff // step, activate, 0)
    gather(4, far, nf)
    finish(4)

    def mlp_out(b, carry):
        at = pl.ds(pl.multiple_of(b * rows, rows), rows)
        part1[at, :] = jnp.dot(b_down[b], hidden[...], preferred_element_type=F32).astype(BF)
        return carry

    lax.fori_loop(0, nf, mlp_out, 0)
    start_pair(1, part1)
    for m in range(5):
        drain(m)
    start_chips(1, part1)
    finish_chips(1, part1, x1, put(own_x))

    def square(i, total):
        v = chunk(own_x, i)
        return total + jnp.sum(v * v, axis=0, keepdims=True)

    mine = lax.fori_loop(0, share // LANES, square, jnp.zeros((1, tokens), F32))
    squares[0] = jnp.broadcast_to(mine, squares.shape[1:])
    for i in range(1, nt):
        s_copy(i).start()
    for i in range(1, nt):
        s_copy(i).wait()
    total = squares[0, pl.ds(0, 1), :]
    for i in range(1, nt):
        total = total + squares[i, pl.ds(0, 1), :]
    factor = lax.rsqrt(total / features + EPS)

    def closing(i, carry):
        gain = column(g_out[pl.ds(t * (share // LANES) + i, 1), :], tokens)
        put(out)(i, chunk(own_x, i) * factor * gain)
        return carry

    lax.fori_loop(0, share // LANES, closing, 0)


def solution(mesh):
    nr, nf, nt = mesh.shape["rep"], mesh.shape["fs"], mesh.shape["tp"]

    def on_device(act, w_in, w_out, w_gate, w_up, w_down, scale, g_mix, g_ffn, g_out):
        features, tokens = act.shape
        rows, channels = w_in.shape
        ff = w_gate.shape[1]
        share = features // nt
        nh = nt // 2
        anywhere = pl.BlockSpec(memory_space=pl.ANY)
        vmem = pl.BlockSpec(memory_space=pltpu.VMEM)
        dma = pltpu.SemaphoreType.DMA
        scratch = [
            pltpu.VMEM((nf, rows, channels), BF),
            pltpu.VMEM((nf, rows, channels), BF),
            pltpu.VMEM((nf, rows, ff), BF),
            pltpu.VMEM((nf, rows, ff), BF),
            pltpu.VMEM((nf, rows, ff), BF),
            pltpu.VMEM((features, tokens), BF),
            pltpu.VMEM((features, tokens), BF),
            pltpu.VMEM((features, tokens), BF),
            pltpu.VMEM((features, tokens), BF),
            pltpu.VMEM((channels, tokens), F32),
            pltpu.VMEM((channels, tokens), BF),
            pltpu.VMEM((ff, tokens), F32),
            pltpu.VMEM((ff, tokens), F32),
            pltpu.VMEM((ff, tokens), BF),
            pltpu.VMEM((share, tokens), F32),
            pltpu.VMEM((nt, 8, tokens), F32),
            pltpu.VMEM((2, nh, share, tokens), BF),
            pltpu.VMEM((2, nh, share, tokens), BF),
            dma((5,)),
            dma((5, 2, 2)),
            dma((5, nf)),
            dma((5, 2, 2, max(nr - 1, 1))),
            dma((5, nf, max(nr - 1, 1))),
            dma((2, nh)), dma((2, nh)), dma((2, nh)), dma((2, nh)),
            dma((nh,)), dma((nh,)), dma((nh,)), dma((nh,)),
            dma((nt,)), dma((nt,)),
        ]
        return pl.pallas_call(
            functools.partial(body, nr, nf, nt),
            out_shape=jax.ShapeDtypeStruct((share, tokens), BF),
            in_specs=[vmem] + [anywhere] * 5 + [vmem] * 4,
            out_specs=vmem,
            scratch_shapes=scratch,
            compiler_params=pltpu.CompilerParams(
                collective_id=0, has_side_effects=True, vmem_limit_bytes=60 * 1024 * 1024
            ),
        )(
            act, w_in, w_out, w_gate, w_up, w_down,
            *[v.reshape(-1, LANES) for v in (scale, g_mix, g_ffn, g_out)],
        )

    weight = P("fs", "tp")
    tokens_split = P(None, ("rep", "fs"))
    return jax.shard_map(
        on_device,
        mesh=mesh,
        in_specs=(tokens_split, *[weight] * 5, P(), P(), P(), P()),
        out_specs=P("tp", ("rep", "fs")),
        check_vma=False,
    )
```

```python
import functools

import jax
import jax.numpy as jnp
from jax import lax
from jax.experimental import pallas as pl
from jax.experimental.pallas import tpu as pltpu
from jax.sharding import PartitionSpec as P

POOL_GROUP = 256
SEQ_LEN = 256
EPS = 1e-06
LANES = 128
MESH = pl.DeviceIdType.MESH
BF = jnp.bfloat16
F32 = jnp.float32


def dot_first(weights, acts):
    return lax.dot_general(weights, acts, (((0,), (0,)), ((), ())), preferred_element_type=F32)


def column(row, width):
    square = jnp.transpose(jnp.broadcast_to(row, (LANES, LANES)))
    return jnp.concatenate([square] * (width // LANES), axis=1)


def body(
    nr, nf, nt,
    act, w_in, w_out, w_gate, w_up, w_down, scale, g_mix, g_ffn, g_out, out,
    b_in, b_out, b_gate, b_up, b_down,
    h, x1, part0, part1, u_acc, pooled, gate_acc, up_acc, hidden, own_x, squares,
    buf_a, buf_b,
    own_sem, zsend, zrecv, ysend, yrecv,
    a_send, a_recv, b_send, b_recv, c_send, c_recv, d_send, d_recv, s_send, s_recv,
):
    r, f, t = lax.axis_index("rep"), lax.axis_index("fs"), lax.axis_index("tp")
    features, tokens = act.shape
    shards = (w_in, w_out, w_gate, w_up, w_down)
    full = (b_in, b_out, b_gate, b_up, b_down)
    rows = w_in.shape[0]
    piece = rows // nr
    share = features // nt
    channels = w_in.shape[1]
    ff = w_gate.shape[1]
    nh = nt // 2
    chip, parity = t // 2, lax.rem(t, 2)
    partner = t + 1 - 2 * parity

    cut = -(-ff // (2 * LANES)) * LANES
    items = [(0, 0, channels), (1, 0, channels)]
    for m in (2, 3, 4):
        items += [(m, 0, cut), (m, cut, ff - cut)]

    own = [pltpu.make_async_copy(shards[m], full[m].at[f], own_sem.at[m]) for m in range(5)]
    for copy in own:
        copy.start()

    barrier = pltpu.get_barrier_semaphore()
    for step in (1, nf - 1):
        pl.semaphore_signal(barrier, inc=1, device_id=(r, lax.rem(f + step, nf), t), device_id_type=MESH)
    for o in range(1, nr):
        pl.semaphore_signal(barrier, inc=1, device_id=(lax.rem(r + o, nr), f, t), device_id_type=MESH)
    for i in range(1, nt):
        pl.semaphore_signal(barrier, inc=1, device_id=(r, f, lax.rem(t + i, nt)), device_id_type=MESH)
    pl.semaphore_wait(barrier, 2 + (nr - 1) + (nt - 1))

    def part_of(m, blk, of):
        matrix, start, size = items[m]
        at = pl.ds(pl.multiple_of(of * piece, piece), piece)
        return full[matrix].at[blk, at, pl.ds(start, size)]

    def z_copy(m, blk, way, d):
        ref = part_of(m, blk, r)
        return pltpu.make_async_remote_copy(
            src_ref=ref, dst_ref=ref,
            send_sem=zsend.at[m, way, lax.rem(d, 2)], recv_sem=zrecv.at[m, blk],
            device_id=(r, f + 1 - 2 * way, t), device_id_type=MESH,
        )

    def y_copy(m, blk, way, d, o):
        ref = part_of(m, blk, r)
        return pltpu.make_async_remote_copy(
            src_ref=ref, dst_ref=ref,
            send_sem=ysend.at[m, way, lax.rem(d, 2), o - 1], recv_sem=yrecv.at[m, blk, o - 1],
            device_id=(lax.rem(r + o, nr), f, t), device_id_type=MESH,
        )

    def y_arrival(m, blk, o):
        source = lax.rem(r - o + nr, nr)
        ref = part_of(m, blk, source)
        return pltpu.make_async_remote_copy(
            src_ref=ref, dst_ref=ref,
            send_sem=ysend.at[m, 0, 0, o - 1], recv_sem=yrecv.at[m, blk, o - 1],
            device_id=(lax.rem(r + o, nr), f, t), device_id_type=MESH,
        )

    can_send = (f + 1 < nf, f >= 1)
    hops = (f, nf - 1 - f)

    def send_own(m):
        if items[m][1] == 0:
            own[items[m][0]].wait()
        for way in (0, 1):
            @pl.when(can_send[way])
            def _():
                z_copy(m, f, way, 0).start()

    def arrival(m, way, d):
        blk = f - d if way == 0 else f + d

        @pl.when(d <= hops[way])
        def _():
            z_copy(m, blk, way, d).wait_recv()

            @pl.when(can_send[way])
            def _():
                @pl.when(d >= 2)
                def _():
                    z_copy(m, blk, way, d).wait_send()

                z_copy(m, blk, way, d).start()

            for o in range(1, nr):
                @pl.when(d >= 3)
                def _():
                    y_copy(m, blk, way, d, o).wait_send()

                y_copy(m, blk, way, d, o).start()

    def gather(m, low, high):
        if low >= high:
            return

        def rounds(d, carry):
            arrival(m, 0, d)
            arrival(m, 1, d)
            return carry

        if low == 1:
            rounds(jnp.int32(1), 0)
            if m + 1 < len(items):
                send_own(m + 1)
            low = 2
        lax.fori_loop(low, high, rounds, 0)

    def finish(m):
        def one(blk, carry):
            @pl.when(blk != f)
            def _():
                for o in range(1, nr):
                    y_arrival(m, blk, o).wait_recv()
            return carry

        lax.fori_loop(0, nf, one, 0)

    def drain(m):
        for way in (0, 1):
            for back in (0, 1):
                last = hops[way] - back

                @pl.when(jnp.logical_and(can_send[way], last >= 0))
                def _():
                    z_copy(m, f, way, last).wait_send()

                @pl.when(last >= 1)
                def _():
                    for o in range(1, nr):
                        y_copy(m, f, way, last, o).wait_send()

    def share_of(ref, j):
        return ref.at[pl.ds(pl.multiple_of(j * share, share), share), :]

    def normalize(load, gain, store, count):
        def square(i, total):
            v = load(i)
            return total + jnp.sum(v * v, axis=0, keepdims=True)

        total = lax.fori_loop(0, count, square, jnp.zeros((1, tokens), F32))
        factor = lax.rsqrt(total / features + EPS)

        def scaled(i, carry):
            store(i, load(i) * factor * column(gain[pl.ds(i, 1), :], tokens))
            return carry

        lax.fori_loop(0, count, scaled, 0)

    def chunk(ref, i):
        return ref[pl.ds(pl.multiple_of(i * LANES, LANES), LANES), :].astype(F32)

    def put(ref):
        def store(i, v):
            ref[pl.ds(pl.multiple_of(i * LANES, LANES), LANES), :] = v.astype(ref.dtype)
        return store

    def a_copy(k, part, c):
        return pltpu.make_async_remote_copy(
            src_ref=share_of(part, 2 * c + 1 - parity), dst_ref=buf_a.at[k, c],
            send_sem=a_send.at[k, c], recv_sem=a_recv.at[k, c],
            device_id=(r, f, partner), device_id_type=MESH,
        )

    def b_copy(k, part, i):
        target = 2 * lax.rem(chip + i, nh) + parity
        return pltpu.make_async_remote_copy(
            src_ref=share_of(part, target), dst_ref=buf_b.at[k, i],
            send_sem=b_send.at[k, i], recv_sem=b_recv.at[k, i],
            device_id=(r, f, target), device_id_type=MESH,
        )

    def start_pair(k, part):
        for i in range(nh):
            a_copy(k, part, i).start()

    def start_chips(k, part):
        for i in range(1, nh):
            c = lax.rem(chip + i, nh)
            target = 2 * c + parity
            a_copy(k, part, c).wait()

            def add(n, carry):
                at = pl.ds(pl.multiple_of(target * share + n * LANES, LANES), LANES)
                mine = part[at, :].astype(F32)
                theirs = buf_a[k, c, pl.ds(pl.multiple_of(n * LANES, LANES), LANES), :].astype(F32)
                part[at, :] = (mine + theirs).astype(BF)
                return carry

            lax.fori_loop(0, share // LANES, add, 0)
            b_copy(k, part, i).start()

    def finish_chips(k, part, base, store):
        a_copy(k, part, chip).wait()
        for i in range(1, nh):
            b_copy(k, part, i).wait()

        def add(n, carry):
            here = pl.ds(pl.multiple_of(n * LANES, LANES), LANES)
            at = pl.ds(pl.multiple_of(t * share + n * LANES, LANES), LANES)
            total = part[at, :].astype(F32) + buf_a[k, chip, here, :].astype(F32)
            for i in range(1, nh):
                total = total + buf_b[k, i, here, :].astype(F32)
            store(n, base[at, :].astype(F32) + total)
            return carry

        lax.fori_loop(0, share // LANES, add, 0)

    def c_copy(i):
        ref = share_of(x1, t)
        return pltpu.make_async_remote_copy(
            src_ref=ref, dst_ref=ref, send_sem=c_send.at[i], recv_sem=c_recv.at[i],
            device_id=(r, f, 2 * lax.rem(chip + i, nh) + parity), device_id_type=MESH,
        )

    def d_copy(i):
        ref = share_of(x1, 2 * lax.rem(chip - i + nh, nh) + parity)
        return pltpu.make_async_remote_copy(
            src_ref=ref, dst_ref=ref, send_sem=d_send.at[i], recv_sem=d_recv.at[i],
            device_id=(r, f, partner), device_id_type=MESH,
        )

    def s_copy(i):
        return pltpu.make_async_remote_copy(
            src_ref=squares.at[0], dst_ref=squares.at[i], send_sem=s_send.at[i], recv_sem=s_recv.at[i],
            device_id=(r, f, lax.rem(t + i, nt)), device_id_type=MESH,
        )

    send_own(0)
    normalize(functools.partial(chunk, act), g_mix, put(h), features // LANES)

    gather(0, 1, nf)
    gather(1, 1, nf)
    finish(0)
    u_acc[...] = jnp.zeros_like(u_acc)

    def mix_in(b, carry):
        at = pl.ds(pl.multiple_of(b * rows, rows), rows)
        u_acc[...] += dot_first(b_in[b], h[at, :])
        return carry

    lax.fori_loop(0, nf, mix_in, 0)
    for i in range(channels // LANES):
        first = t * channels + i * LANES
        window = jnp.int32(2) << (first // POOL_GROUP)
        behind = window // 2
        onward = window - behind
        source = lax.broadcasted_iota(jnp.int32, (SEQ_LEN, SEQ_LEN), 0)
        place = lax.broadcasted_iota(jnp.int32, (SEQ_LEN, SEQ_LEN), 1)
        inside = jnp.logical_and(source >= place - behind, source < place + onward)
        band = jnp.where(inside, 1.0, 0.0).astype(BF)
        spot = lax.broadcasted_iota(jnp.int32, (1, SEQ_LEN), 1)
        count = (jnp.minimum(spot + onward, SEQ_LEN) - jnp.maximum(spot - behind, 0)).astype(F32)
        gain = column(scale[pl.ds(first // LANES, 1), :], SEQ_LEN)
        for s in range(tokens // SEQ_LEN):
            at = (pl.ds(i * LANES, LANES), pl.ds(s * SEQ_LEN, SEQ_LEN))
            u = u_acc[at].astype(BF)
            mean = jnp.dot(u, band, preferred_element_type=F32) / count
            pooled[at] = ((mean - u.astype(F32)) * gain).astype(BF)

    gather(2, 1, nf)
    finish(1)

    def mix_out(b, carry):
        at = pl.ds(pl.multiple_of(b * rows, rows), rows)
        part0[at, :] = jnp.dot(b_out[b], pooled[...], preferred_element_type=F32).astype(BF)
        return carry

    lax.fori_loop(0, nf, mix_out, 0)
    start_pair(0, part0)
    gather(3, 1, nf)
    start_chips(0, part0)
    gather(4, 1, nf)

    def keep_x1(n, v):
        at = pl.ds(pl.multiple_of(t * share + n * LANES, LANES), LANES)
        x1[at, :] = v.astype(BF)

    finish_chips(0, part0, act, keep_x1)
    for i in range(1, nh):
        c_copy(i).start()
    d_copy(0).start()
    gather(5, 1, nf)
    for i in range(1, nh):
        c_copy(i).wait()
        d_copy(i).start()
    gather(6, 1, nf)
    for i in range(nh):
        d_copy(i).wait()
    normalize(functools.partial(chunk, x1), g_ffn, put(h), features // LANES)
    finish(2)
    finish(3)
    gate_acc[...] = jnp.zeros_like(gate_acc)
    up_acc[...] = jnp.zeros_like(up_acc)

    def project(source, acc):
        def one(b, carry):
            at = pl.ds(pl.multiple_of(b * rows, rows), rows)
            acc[...] += dot_first(source[b], h[at, :])
            return carry

        lax.fori_loop(0, nf, one, 0)

    gather(7, 1, nf)
    project(b_gate, gate_acc)
    finish(4)
    finish(5)
    project(b_up, up_acc)
    step = 32

    def activate(n, carry):
        at = pl.ds(pl.multiple_of(n * step, step), step)
        v = gate_acc[at, :]
        hidden[at, :] = (v / (1.0 + jnp.exp(-v)) * up_acc[at, :]).astype(BF)
        return carry

    lax.fori_loop(0, ff // step, activate, 0)
    finish(6)
    finish(7)

    def mlp_out(b, carry):
        at = pl.ds(pl.multiple_of(b * rows, rows), rows)
        part1[at, :] = jnp.dot(b_down[b], hidden[...], preferred_element_type=F32).astype(BF)
        return carry

    if share % rows == 0:
        blocks = share // rows

        def pair_out(c):
            theirs, ours = 2 * c + 1 - parity, 2 * c + parity
            lax.fori_loop(theirs * blocks, (theirs + 1) * blocks, mlp_out, 0)
            a_copy(1, part1, c).start()
            lax.fori_loop(ours * blocks, (ours + 1) * blocks, mlp_out, 0)

        for i in range(1, nh):
            pair_out(lax.rem(chip + i, nh))
        start_chips(1, part1)
        pair_out(chip)
    else:
        lax.fori_loop(0, nf, mlp_out, 0)
        start_pair(1, part1)
        start_chips(1, part1)
    for m in range(len(items)):
        drain(m)
    finish_chips(1, part1, x1, put(own_x))

    def square(i, total):
        v = chunk(own_x, i)
        return total + jnp.sum(v * v, axis=0, keepdims=True)

    mine = lax.fori_loop(0, share // LANES, square, jnp.zeros((1, tokens), F32))
    squares[0] = jnp.broadcast_to(mine, squares.shape[1:])
    for i in range(1, nt):
        s_copy(i).start()
    for i in range(1, nt):
        s_copy(i).wait()
    total = squares[0, pl.ds(0, 1), :]
    for i in range(1, nt):
        total = total + squares[i, pl.ds(0, 1), :]
    factor = lax.rsqrt(total / features + EPS)

    def closing(i, carry):
        gain = column(g_out[pl.ds(t * (share // LANES) + i, 1), :], tokens)
        put(out)(i, chunk(own_x, i) * factor * gain)
        return carry

    lax.fori_loop(0, share // LANES, closing, 0)


def solution(mesh):
    nr, nf, nt = mesh.shape["rep"], mesh.shape["fs"], mesh.shape["tp"]

    def on_device(act, w_in, w_out, w_gate, w_up, w_down, scale, g_mix, g_ffn, g_out):
        features, tokens = act.shape
        rows, channels = w_in.shape
        ff = w_gate.shape[1]
        share = features // nt
        nh = nt // 2
        anywhere = pl.BlockSpec(memory_space=pl.ANY)
        vmem = pl.BlockSpec(memory_space=pltpu.VMEM)
        dma = pltpu.SemaphoreType.DMA
        scratch = [
            pltpu.VMEM((nf, rows, channels), BF),
            pltpu.VMEM((nf, rows, channels), BF),
            pltpu.VMEM((nf, rows, ff), BF),
            pltpu.VMEM((nf, rows, ff), BF),
            pltpu.VMEM((nf, rows, ff), BF),
            pltpu.VMEM((features, tokens), BF),
            pltpu.VMEM((features, tokens), BF),
            pltpu.VMEM((features, tokens), BF),
            pltpu.VMEM((features, tokens), BF),
            pltpu.VMEM((channels, tokens), F32),
            pltpu.VMEM((channels, tokens), BF),
            pltpu.VMEM((ff, tokens), F32),
            pltpu.VMEM((ff, tokens), F32),
            pltpu.VMEM((ff, tokens), BF),
            pltpu.VMEM((share, tokens), F32),
            pltpu.VMEM((nt, 8, tokens), F32),
            pltpu.VMEM((2, nh, share, tokens), BF),
            pltpu.VMEM((2, nh, share, tokens), BF),
            dma((5,)),
            dma((8, 2, 2)),
            dma((8, nf)),
            dma((8, 2, 2, max(nr - 1, 1))),
            dma((8, nf, max(nr - 1, 1))),
            dma((2, nh)), dma((2, nh)), dma((2, nh)), dma((2, nh)),
            dma((nh,)), dma((nh,)), dma((nh,)), dma((nh,)),
            dma((nt,)), dma((nt,)),
        ]
        return pl.pallas_call(
            functools.partial(body, nr, nf, nt),
            out_shape=jax.ShapeDtypeStruct((share, tokens), BF),
            in_specs=[vmem] + [anywhere] * 5 + [vmem] * 4,
            out_specs=vmem,
            scratch_shapes=scratch,
            compiler_params=pltpu.CompilerParams(
                collective_id=0, has_side_effects=True, vmem_limit_bytes=60 * 1024 * 1024
            ),
        )(
            act, w_in, w_out, w_gate, w_up, w_down,
            *[v.reshape(-1, LANES) for v in (scale, g_mix, g_ffn, g_out)],
        )

    weight = P("fs", "tp")
    tokens_split = P(None, ("rep", "fs"))
    return jax.shard_map(
        on_device,
        mesh=mesh,
        in_specs=(tokens_split, *[weight] * 5, P(), P(), P(), P()),
        out_specs=P("tp", ("rep", "fs")),
        check_vma=False,
    )
```
